32 devices in a mesh: ep: 8 (over z, x), tp: 4 (over y, core).
Axes of the slice: x: 2, y: 2, z: 4, core: 2. Of those that a mesh axis runs over, the one named last changes fastest.
Arguments:
- mixer_input: bfloat16 [4096, 2048], P('ep'), may hold values from -6 to 6
- mixer_gain: float32 [2048], replicated, may hold values from 0.1 to 1.9
- query_weight: bfloat16 [2048, 1024], P(None, 'tp'), may hold values from -0.125 to 0.125
- key_weight: bfloat16 [2048, 1024], P(None, 'tp'), may hold values from -0.125 to 0.125
- value_weight: bfloat16 [2048, 1024], P(None, 'tp'), may hold values from -0.125 to 0.125
- gate_weight: bfloat16 [2048, 1024], P(None, 'tp'), may hold values from -0.125 to 0.125
- head_gain: float32 [1024], P('tp'), may hold values from 0.1 to 1.9
- output_weight: bfloat16 [1024, 2048], P('tp'), may hold values from -0.1875 to 0.1875
- log_decay: float32 [4096, 8], P('ep', 'tp'), may hold values from -1 to 0, as said below
- expert_input: bfloat16 [4096, 2048], P(('ep', 'tp')), may hold values from -6 to 6
- expert_gain: float32 [2048], replicated, may hold values from 0.1 to 1.9
- routes: int32 [4096, 2], P(('ep', 'tp')), may hold values from 0 to 7, all different within a row; in each aligned block of 128 rows (0 to 127, 128 to 255, ...) at most 48 rows name the same one
- route_weight: float32 [4096, 2], P(('ep', 'tp')), may hold values from 0.1 to 1
- expert_gate: bfloat16 [8, 2048, 1024], P('ep', None, 'tp'), may hold values from -0.125 to 0.125
- expert_up: bfloat16 [8, 2048, 1024], P('ep', None, 'tp'), may hold values from -0.125 to 0.125
- expert_down: bfloat16 [8, 1024, 2048], P('ep', 'tp'), may hold values from -0.1875 to 0.1875
Outputs:
- mixer_output: bfloat16 [4096, 2048], P(('ep', 'tp'))
- expert_output: bfloat16 [4096, 2048], P(('ep', 'tp'))
The draws below stay inside these ranges and needn't reach their ends.
Inputs may be any that keep to these rules, and one draw needn't show every extreme that they name: `routes`: each row names 2 different experts. Among the rows of one device no expert is named more than 48 times, and in every draw the rows of some device name some expert exactly 48 times. `log_decay`: negative values.
All inputs are finite; a program needn't handle non-finite values.
Results may differ from the reference program's by a relative error of at most 0.025.
Values may be sent and summed in bfloat16 or wider, within the bound.
A program may use at most 128 MiB of HBM per device.

```python
import math
import jax
import jax.numpy as jnp
import numpy as np
from jax import lax

D = 2048
HEADS = 8
HEAD_DIM = 128
FF = 1024
BLOCK = 128
TOPK = 2
TOK_A = 512
TOK_B = 128
RET_WIDTH = 1024
TOKENS_A = 4096
TOKENS_B = 4096
EXPERTS = 8
CAP = 48
N_EP = 8
N_TP = 4


def draw_log_decay(key, part):
    symbol_strings = jax.random.split(key, 7)
    series_extent = TOKENS_A
    fast_share = 50
    fast_heads = jax.random.randint(symbol_strings[0], (HEADS,), 0, 100) < fast_share
    fast_rate = 1.0 / jax.random.uniform(symbol_strings[1], (HEADS,), jnp.float32, 30.0, 60.0)
    slow_rate = 2.302585 * jax.random.uniform(symbol_strings[2], (HEADS,), jnp.float32, 0.3, 1.0) / (2.5 * series_extent)
    rate = jnp.where(fast_heads, fast_rate, slow_rate)
    shard_factor = jnp.repeat(jax.random.uniform(symbol_strings[3], (N_EP,), jnp.float32, 1.0, 2.5), TOK_A)
    rough = jax.random.uniform(symbol_strings[4], (series_extent, HEADS), jnp.float32, 0.5, 1.5)
    default_fading_exponent = -rate[None, :] * shard_factor[:, None] * rough
    spike_offset = jax.random.randint(symbol_strings[5], (3,), 0, series_extent)
    objective_scores = jax.random.uniform(symbol_strings[6], (3, HEADS), jnp.float32, 0.2, 0.4)
    agreeing_tally = (jnp.arange(series_extent, dtype=jnp.int32)[:, None] == spike_offset[None, :]).astype(jnp.float32)
    spike_clusters = jnp.sum(agreeing_tally[:, :, None] * jnp.log(1.0 - objective_scores)[None, :, :], axis=1)
    return (default_fading_exponent + spike_clusters).astype(jnp.float32)


def block_scale(key, extent, pieces, least, top_value):
    def one(dim, parts):
        heights = jax.random.uniform(jax.random.fold_in(jax.random.fold_in(key, 6), dim), (parts,), jnp.float32, least / len(pieces), top_value / len(pieces))
        return jnp.repeat(jnp.exp(heights), extent[dim] // parts).reshape((-1,) + (1,) * (len(extent) - dim - 1))

    loudness = one(*pieces[0])
    for cut in pieces[1:]:
        loudness = loudness * one(*cut)
    return loudness


def routed_block(own_key, own, number, rows, count, top, bound, lean):
    ranking = jax.random.permutation(own_key, count)
    packed, common = shares(count, rows * top, bound, lean, True), shares(count, rows * top, bound, lean, False)
    places = jnp.arange(count)

    def named(tallies, rotation):
        used = int((tallies > 0).sum())
        fixed = max(1, used // 4)
        moved = fixed + (places - fixed + rotation * (used - fixed)) % max(1, count - fixed)
        return jnp.zeros((count,), jnp.int32).at[ranking[jnp.where(places < fixed, places, moved)]].set(jnp.asarray(tallies, jnp.int32))

    tallies = jnp.where(number % 4 == 0, named(packed, number // 4), named(common, number - number // 4 - 1))
    mixed = jax.random.permutation(jax.random.fold_in(own, 3), count)
    donor, taker = mixed[0:count // 2 * 2:2], mixed[1:count // 2 * 2:2]
    margin = jnp.minimum(tallies[donor] - 1, bound - tallies[taker]) // 2
    margin = jnp.where((donor == ranking[0]) | (taker == ranking[0]) | (tallies[taker] == 0), 0, jnp.maximum(margin, 0))
    moved = jax.random.randint(jax.random.fold_in(own, 4), (count // 2,), 0, 1 << 20) % (margin + 1)
    tallies = tallies.at[donor].add(-moved).at[taker].add(moved)
    labels = jnp.searchsorted(jnp.cumsum(tallies), jnp.arange(rows * top), side="right").astype(jnp.int32)
    listing = labels.reshape(top, rows).T
    listing = listing[jax.random.permutation(jax.random.fold_in(own, 1), rows)]
    rotation = jax.random.randint(jax.random.fold_in(own, 2), (rows, 1), 0, top)
    return jnp.take_along_axis(listing, (jnp.arange(top)[None, :] + rotation) % top, axis=1)


def shares(number_of, total, most, skew, full):
    portions = [(1 << 20) // math.isqrt(standing ** skew) + 1 for standing in range(1, number_of + 1)]
    largest = most if full else min(most, max(-(-total // number_of), total * portions[0] // sum(portions)))
    least = 1 if total - largest >= number_of - 1 else 0
    given, spare = [largest] + [least] * (number_of - 1), total - largest - least * (number_of - 1)
    while spare > 0:
        candidates = [i for i in range(1, number_of) if given[i] < largest] or [i for i in range(1, number_of) if given[i] < most]
        mass, budget = sum([portions[i] for i in candidates]), spare
        for i in candidates:
            more = min(most - given[i], max(1, budget * portions[i] // mass), spare)
            given[i] = given[i] + more
            spare = spare - more
    return np.array(given)


def gaussian(rng, dims, deviation, most, pieces=(), held_as=jnp.bfloat16):
    values = deviation * jax.random.normal(rng, dims, jnp.float32)
    if pieces:
        values = values * block_scale(rng, dims, pieces, -0.22, 0.18)
    return jnp.clip(values, -most, most).astype(held_as)


def setup_inputs(seed: int = 0) -> dict:
    splits = jax.random.split(jax.random.key(seed), 17)
    mixer_input = gaussian(splits[0], (TOKENS_A, D), 1.0, 6.0, ((0, 8),))
    mixer_gain = jnp.clip(1.0 + 0.18 * jax.random.normal(splits[1], (D,), jnp.float32), 0.1, 1.9)
    query_weight = gaussian(splits[2], (D, RET_WIDTH), D ** -0.5, 0.125, ((1, 4),))
    key_weight = gaussian(splits[3], (D, RET_WIDTH), D ** -0.5, 0.125, ((1, 4),))
    value_weight = gaussian(splits[4], (D, RET_WIDTH), D ** -0.5, 0.125, ((1, 4),))
    gate_weight = gaussian(splits[5], (D, RET_WIDTH), D ** -0.5, 0.125, ((1, 4),))
    head_gain = jnp.clip(1.0 + 0.18 * jax.random.normal(splits[6], (RET_WIDTH,), jnp.float32), 0.1, 1.9)
    output_weight = gaussian(splits[7], (RET_WIDTH, D), RET_WIDTH ** -0.5, 0.1875, ((0, 4),))
    log_decay = draw_log_decay(jax.random.fold_in(splits[16], 71), 0)
    expert_input = gaussian(splits[9], (TOKENS_B, D), 1.0, 6.0, ((0, 32),))
    expert_gain = jnp.clip(1.0 + 0.18 * jax.random.normal(splits[10], (D,), jnp.float32), 0.1, 1.9)
    routes_keys = jax.random.split(jax.random.fold_in(splits[11], 1), TOKENS_B // TOK_B)
    routes_turns = jax.random.permutation(jax.random.fold_in(splits[11], 3), TOKENS_B // TOK_B)
    routes = jax.vmap(lambda own, number: routed_block(jax.random.fold_in(splits[11], 2), own, number, TOK_B, EXPERTS, TOPK, CAP, 1))(routes_keys, routes_turns).reshape((TOKENS_B, TOPK))
    route_weight = jnp.clip(0.1 + 0.9 * jax.random.uniform(splits[12], (TOKENS_B, TOPK), jnp.float32) ** block_scale(splits[12], (TOKENS_B, TOPK), ((0, 32),), -0.2, 0.2), 0.1, 1.0)
    expert_gate = gaussian(splits[13], (EXPERTS, D, FF), D ** -0.5, 0.125, ((0, 8), (2, 4)))
    expert_up = gaussian(splits[14], (EXPERTS, D, FF), D ** -0.5, 0.125, ((0, 8), (2, 4)))
    expert_down = gaussian(splits[15], (EXPERTS, FF, D), FF ** -0.5, 0.1875, ((0, 8), (1, 4)))
    return dict(mixer_input=mixer_input, mixer_gain=mixer_gain, query_weight=query_weight, key_weight=key_weight, value_weight=value_weight, gate_weight=gate_weight, head_gain=head_gain, output_weight=output_weight, log_decay=log_decay, expert_input=expert_input, expert_gain=expert_gain, routes=routes, route_weight=route_weight, expert_gate=expert_gate, expert_up=expert_up, expert_down=expert_down)


EPS = 1e-06
HIGH = lax.Precision.HIGHEST

def norm_rows(values, gain):
    floats = values.astype(jnp.float32)
    scale = lax.rsqrt(lax.optimization_barrier(jnp.mean(floats * floats, axis=-1, keepdims=True)) + EPS)
    return (floats * scale * gain).astype(jnp.bfloat16)

def rotate(values, position):
    half_dim = values.shape[-1] // 2
    frequency = 10000.0 ** (-jnp.arange(half_dim, dtype=jnp.float32) / half_dim)
    angles = position.astype(jnp.float32)[:, None] * frequency[None, :]
    cosine = jnp.cos(angles)[:, None, :]
    sine_part = jnp.sin(angles)[:, None, :]
    first_half = values[..., :half_dim]
    second = values[..., half_dim:]
    return jnp.concatenate([first_half * cosine - second * sine_part, first_half * sine_part + second * cosine], axis=-1)

def lifted(array):
    return lax.optimization_barrier(array).astype(jnp.float32)

def retain(q_rot, k_rot, values_new, log_decay):
    series_extent, head_count, head_dim = q_rot.shape
    block_count = series_extent // BLOCK
    row_ids = lax.broadcasted_iota(jnp.int32, (BLOCK, BLOCK), 0)
    col_ids = lax.broadcasted_iota(jnp.int32, (BLOCK, BLOCK), 1)
    lower_mask = col_ids <= row_ids
    triangle = lower_mask.astype(jnp.float32)

    def shaped(array):
        return array.reshape((block_count, BLOCK) + array.shape[1:])

    def advance(carry_state, inputs):
        q_block, k_block, v_block, step_block = inputs
        cumulative = jnp.einsum('ij,jh->hi', triangle, step_block, precision=HIGH)
        block_total = cumulative[:, -1]
        differences = cumulative[:, :, None] - cumulative[:, None, :]
        decays = jnp.where(lower_mask, jnp.exp(jnp.where(lower_mask, differences, 0.0)), 0.0)
        q_float = q_block.astype(jnp.float32)
        k_float = k_block.astype(jnp.float32)
        v_float = v_block.astype(jnp.float32)
        scores = jnp.einsum('ihd,jhd->hij', q_float, k_float, precision=HIGH)
        weights = lifted((scores * decays).astype(jnp.bfloat16))
        inner_term = jnp.einsum('hij,jhe->ihe', weights, v_float, precision=HIGH)
        cross_term = jnp.einsum('hi,ihd,hde->ihe', jnp.exp(cumulative), q_float, carry_state, precision=HIGH)
        key_scale = jnp.exp(block_total[:, None] - cumulative)
        updates = jnp.einsum('hj,jhd,jhe->hde', key_scale, k_float, v_float, precision=HIGH)
        next_state = jnp.exp(block_total)[:, None, None] * carry_state + updates
        return (next_state, inner_term + cross_term)
    initial = jnp.zeros((head_count, head_dim, head_dim), jnp.float32)
    _, outputs = lax.scan(advance, initial, (shaped(q_rot), shaped(k_rot), shaped(values_new), shaped(log_decay)))
    return outputs.reshape(series_extent, head_count, head_dim)

def reference(mixer_input, mixer_gain, query_weight, key_weight, value_weight, gate_weight, head_gain, output_weight, log_decay, expert_input, expert_gain, routes, route_weight, expert_gate, expert_up, expert_down):
    series_extent = mixer_input.shape[0]
    normed = norm_rows(mixer_input, mixer_gain)

    def project(weight):
        return jnp.dot(normed, weight, preferred_element_type=jnp.float32).astype(jnp.bfloat16)
    queries = project(query_weight)
    keys_raw = project(key_weight)
    values_new = project(value_weight)
    gate_raw = project(gate_weight)
    position = jnp.arange(series_extent, dtype=jnp.int32)
    q_rot = rotate(lifted(queries).reshape(series_extent, HEADS, HEAD_DIM), position).astype(jnp.bfloat16)
    k_rot = (rotate(lifted(keys_raw).reshape(series_extent, HEADS, HEAD_DIM), position) * HEAD_DIM ** (-0.5)).astype(jnp.bfloat16)
    retained = retain(q_rot, k_rot, values_new.reshape(series_extent, HEADS, HEAD_DIM), log_decay)
    centre = lax.optimization_barrier(jnp.mean(retained, axis=-1, keepdims=True))
    spread = lax.optimization_barrier(jnp.mean(jnp.square(retained - centre), axis=-1, keepdims=True))
    scaled = (retained - centre) * lax.rsqrt(spread + EPS) * head_gain.reshape(HEADS, HEAD_DIM)
    gated = scaled.reshape(series_extent, RET_WIDTH) * jax.nn.silu(lifted(gate_raw))
    mixer_hidden = gated.astype(jnp.bfloat16)
    quarter = RET_WIDTH // N_TP
    running = jnp.zeros((series_extent, D), jnp.float32)
    for group_index in range(N_TP):
        group_term = jnp.dot(mixer_hidden[:, group_index * quarter:(group_index + 1) * quarter], output_weight[group_index * quarter:(group_index + 1) * quarter], preferred_element_type=jnp.float32)
        running = running + lifted(group_term.astype(jnp.bfloat16))
    mixer_output = running.astype(jnp.bfloat16)
    expert_normed = norm_rows(expert_input, expert_gain)
    block_count = N_EP * N_TP
    entry_count = TOK_B * TOPK
    flat_routes = routes.reshape(block_count, entry_count)
    onehot = (flat_routes[:, :, None] == jnp.arange(EXPERTS, dtype=jnp.int32)[None, None, :]).astype(jnp.int32)
    prior_count = jnp.cumsum(onehot, axis=1) - onehot
    slot_index = lax.optimization_barrier(jnp.sum(prior_count * onehot, axis=2)).astype(jnp.int32)
    block_ids = jnp.broadcast_to(jnp.arange(block_count, dtype=jnp.int32)[:, None], (block_count, entry_count))
    entry_ids = block_ids * entry_count + jnp.arange(entry_count, dtype=jnp.int32)[None, :]
    slot_table = jnp.full((EXPERTS, block_count, CAP), -1, jnp.int32).at[flat_routes, block_ids, slot_index].set(entry_ids)
    norm_weight = route_weight / lax.optimization_barrier(jnp.sum(route_weight, axis=1, keepdims=True))
    flat_weight = norm_weight.reshape(-1)

    def per_expert(running_sum, inputs):
        gate_w, up_w, down_w, id_table = inputs
        id_list = id_table.reshape(-1)
        valid = id_list >= 0
        safe_ids = jnp.where(valid, id_list, 0).astype(jnp.int32)
        tok_index = (safe_ids // TOPK).astype(jnp.int32)
        rows_in = jnp.where(valid[:, None], expert_normed[tok_index], jnp.zeros((), jnp.bfloat16))
        gate_part = jnp.dot(rows_in, gate_w, preferred_element_type=jnp.float32)
        up_part = jnp.dot(rows_in, up_w, preferred_element_type=jnp.float32)
        hidden = (jax.nn.silu(gate_part) * up_part).astype(jnp.bfloat16)
        result = lifted(jnp.dot(hidden, down_w, preferred_element_type=jnp.float32).astype(jnp.bfloat16))
        scale = jnp.where(valid, flat_weight[safe_ids], 0.0)
        return (running_sum.at[tok_index].add(scale[:, None] * result), None)
    total, _ = lax.scan(per_expert, jnp.zeros((TOKENS_B, D), jnp.float32), (expert_gate, expert_up, expert_down, slot_table))
    expert_output = total.astype(jnp.bfloat16)
    return (mixer_output, expert_output)
```

```python
import functools

import jax
import jax.numpy as jnp
from jax import lax
from jax.experimental import pallas as pl
from jax.experimental.pallas import tpu as pltpu
from jax.sharding import PartitionSpec as P

BLOCK = 128


EPS = 1e-06
HIGH = lax.Precision.HIGHEST


def entering_kernel(n, state_ref, decay_ref, out_ref, states, decays, sent, got, sent_d, got_d):
    me = lax.axis_index("ep")
    tp = lax.axis_index("tp")
    barrier = pltpu.get_barrier_semaphore()

    def greet(offset, carry):
        pl.semaphore_signal(
            barrier,
            inc=1,
            device_id=(lax.rem(me + offset, n), tp),
            device_id_type=pl.DeviceIdType.MESH,
        )
        return carry

    lax.fori_loop(1, n, greet, 0)
    pl.semaphore_wait(barrier, n - 1)

    def copies(source, target):
        return (
            pltpu.make_async_remote_copy(
                src_ref=state_ref,
                dst_ref=states.at[source],
                send_sem=sent.at[target],
                recv_sem=got.at[source],
                device_id=(target, tp),
                device_id_type=pl.DeviceIdType.MESH,
            ),
            pltpu.make_async_remote_copy(
                src_ref=decay_ref,
                dst_ref=decays.at[source],
                send_sem=sent_d.at[target],
                recv_sem=got_d.at[source],
                device_id=(target, tp),
                device_id_type=pl.DeviceIdType.MESH,
            ),
        )

    def send(target, carry):
        for copy in copies(me, target):
            copy.start()
        return carry

    lax.fori_loop(me + 1, n, send, 0)
    out_ref[...] = jnp.zeros_like(out_ref)

    def receive(source, carry):
        for copy in copies(source, me):
            copy.wait_recv()
        for head in range(out_ref.shape[0]):
            out_ref[head] = out_ref[head] * decays[source, head, 0:1, :] + states[
                source, head
            ].astype(jnp.float32)
        return carry

    lax.fori_loop(0, me, receive, 0)

    def finish(target, carry):
        for copy in copies(me, target):
            copy.wait_send()
        return carry

    lax.fori_loop(me + 1, n, finish, 0)


def entering_state(decay, state):
    n = lax.axis_size("ep")
    heads, rows, columns = state.shape
    decay_tile = jnp.broadcast_to(decay[:, None, None], (heads, 8, columns))
    return pl.pallas_call(
        functools.partial(entering_kernel, n),
        out_shape=jax.ShapeDtypeStruct(state.shape, jnp.float32),
        in_specs=[pl.BlockSpec(memory_space=pltpu.VMEM)] * 2,
        out_specs=pl.BlockSpec(memory_space=pltpu.VMEM),
        scratch_shapes=[
            pltpu.VMEM((n, heads, rows, columns), jnp.bfloat16),
            pltpu.VMEM((n, heads, 8, columns), jnp.float32),
            pltpu.SemaphoreType.DMA((n,)),
            pltpu.SemaphoreType.DMA((n,)),
            pltpu.SemaphoreType.DMA((n,)),
            pltpu.SemaphoreType.DMA((n,)),
        ],
        compiler_params=pltpu.CompilerParams(
            collective_id=0, has_side_effects=True, vmem_limit_bytes=24 * 1024 * 1024
        ),
        cost_estimate=pl.CostEstimate(
            flops=2 * n * state.size, bytes_accessed=8 * 1024 * 1024, transcendentals=0
        ),
    )(state.astype(jnp.bfloat16), decay_tile)


def norm_rows(values, gain):
    floats = values.astype(jnp.float32)
    scale = lax.rsqrt(jnp.mean(floats * floats, axis=-1, keepdims=True) + EPS)
    return (floats * scale * gain).astype(jnp.bfloat16)


def rotate(values, position):
    half_dim = values.shape[-1] // 2
    frequency = 10000.0 ** (-jnp.arange(half_dim, dtype=jnp.float32) / half_dim)
    angles = position.astype(jnp.float32)[:, None] * frequency[None, :]
    cosine = jnp.cos(angles)[:, None, :]
    sine_part = jnp.sin(angles)[:, None, :]
    first_half = values[..., :half_dim]
    second = values[..., half_dim:]
    return jnp.concatenate(
        [first_half * cosine - second * sine_part, first_half * sine_part + second * cosine],
        axis=-1,
    )


def mixer_half(
    mixer_input,
    mixer_gain,
    query_weight,
    key_weight,
    value_weight,
    gate_weight,
    head_gain,
    output_weight,
    log_decay,
):
    row_count = mixer_input.shape[0]
    head_count = log_decay.shape[1]
    mix_width = query_weight.shape[1]
    head_dim = mix_width // head_count
    normed = norm_rows(mixer_input, mixer_gain)

    def project(weight):
        return jnp.dot(normed, weight, preferred_element_type=jnp.float32).astype(jnp.bfloat16)

    queries = project(query_weight)
    keys_raw = project(key_weight)
    values_new = project(value_weight)
    gate_raw = project(gate_weight)
    position = lax.axis_index("ep") * row_count + jnp.arange(row_count, dtype=jnp.int32)
    q_rot = rotate(
        queries.astype(jnp.float32).reshape(row_count, head_count, head_dim), position
    ).astype(jnp.bfloat16)
    k_rot = (
        rotate(keys_raw.astype(jnp.float32).reshape(row_count, head_count, head_dim), position)
        * head_dim ** (-0.5)
    ).astype(jnp.bfloat16)
    block_count = row_count // BLOCK
    q_blocks = q_rot.reshape(block_count, BLOCK, head_count, head_dim)
    k_blocks = k_rot.reshape(block_count, BLOCK, head_count, head_dim)
    v_blocks = values_new.reshape(block_count, BLOCK, head_count, head_dim)
    log_steps = log_decay.reshape(block_count, BLOCK, head_count)
    row_ids = lax.broadcasted_iota(jnp.int32, (BLOCK, BLOCK), 0)
    col_ids = lax.broadcasted_iota(jnp.int32, (BLOCK, BLOCK), 1)
    lower_mask = col_ids <= row_ids
    cumulative = jnp.einsum(
        "ij,bjh->bhi", lower_mask.astype(jnp.float32), log_steps, precision=HIGH
    )
    block_total = cumulative[:, :, -1]
    differences = cumulative[:, :, :, None] - cumulative[:, :, None, :]
    decays = jnp.where(lower_mask, jnp.exp(jnp.where(lower_mask, differences, 0.0)), 0.0)
    scores = jnp.einsum("bihd,bjhd->bhij", q_blocks, k_blocks, preferred_element_type=jnp.float32)
    weights = (scores * decays).astype(jnp.bfloat16)
    inner_term = jnp.einsum(
        "bhij,bjhe->bihe", weights, v_blocks, preferred_element_type=jnp.float32
    )
    key_scale = jnp.exp(block_total[:, :, None] - cumulative)
    updates = jnp.einsum(
        "bhj,bjhd,bjhe->bhde",
        key_scale,
        k_blocks.astype(jnp.float32),
        v_blocks.astype(jnp.float32),
        precision=HIGH,
    )
    factor = jnp.exp(block_total)
    local_state = jnp.zeros((head_count, head_dim, head_dim), jnp.float32)
    for block_index in range(block_count):
        local_state = factor[block_index][:, None, None] * local_state + updates[block_index]
    carry_state = entering_state(jnp.exp(jnp.sum(block_total, axis=0)), local_state)
    starts = []
    for block_index in range(block_count):
        starts.append(carry_state)
        carry_state = factor[block_index][:, None, None] * carry_state + updates[block_index]
    carried = jnp.stack(starts)
    cross_term = jnp.einsum(
        "bhi,bihd,bhde->bihe",
        jnp.exp(cumulative),
        q_blocks.astype(jnp.float32),
        carried,
        precision=HIGH,
    )
    retained = (inner_term + cross_term).reshape(row_count, head_count, head_dim)
    centre = jnp.mean(retained, axis=-1, keepdims=True)
    spread = jnp.mean(jnp.square(retained - centre), axis=-1, keepdims=True)
    scaled = (retained - centre) * lax.rsqrt(spread + EPS) * head_gain.reshape(head_count, head_dim)
    mixer_hidden = (
        scaled.reshape(row_count, mix_width) * jax.nn.silu(gate_raw.astype(jnp.float32))
    ).astype(jnp.bfloat16)
    return lax.psum_scatter(
        jnp.dot(mixer_hidden, output_weight, preferred_element_type=jnp.float32).astype(
            jnp.bfloat16
        ),
        "tp",
        scatter_dimension=0,
        tiled=True,
    )


def gathered_pieces(shard):
    peers = lax.axis_size("tp")
    pieces = [shard]
    bit = peers // 2
    while bit:
        pairs = [(i, i ^ bit) for i in range(peers)]
        pieces = pieces + [lax.ppermute(piece, "tp", pairs) for piece in pieces]
        bit //= 2
    return pieces


def expert_half(
    expert_input, expert_gain, routes, route_weight, expert_gate, expert_up, expert_down
):
    tok_count, top_count = routes.shape
    experts = lax.axis_size("ep")
    capacity = max(2, 3 * tok_count * top_count // (2 * experts))
    width = expert_input.shape[1]
    normed = norm_rows(expert_input, expert_gain)
    flat_routes = routes.reshape(-1)
    entries = flat_routes.shape[0]
    onehot = (flat_routes[:, None] == jnp.arange(experts, dtype=jnp.int32)[None, :]).astype(
        jnp.bfloat16
    )
    before = (
        lax.broadcasted_iota(jnp.int32, (entries, entries), 1)
        < lax.broadcasted_iota(jnp.int32, (entries, entries), 0)
    ).astype(jnp.bfloat16)
    prior_count = jnp.dot(before, onehot, preferred_element_type=jnp.float32)
    slot_index = jnp.sum(prior_count * onehot.astype(jnp.float32), axis=1).astype(jnp.int32)
    target = flat_routes * capacity + slot_index
    token_ids = jnp.arange(entries, dtype=jnp.int32) // top_count
    slot_table = jnp.full((experts * capacity,), tok_count, jnp.int32).at[target].set(token_ids)
    padded = jnp.concatenate([normed, jnp.zeros((1, width), jnp.bfloat16)], axis=0)
    outgoing = jnp.take(padded, slot_table, axis=0).reshape(experts, capacity, width)
    arrived = lax.all_to_all(outgoing, "ep", split_axis=0, concat_axis=0, tiled=True)
    sources = arrived.shape[0]
    flat_rows = arrived.reshape(sources * capacity, width)
    gates = gathered_pieces(expert_gate[0])
    ups = gathered_pieces(expert_up[0])
    downs = gathered_pieces(expert_down[0])
    reduced = jnp.zeros((flat_rows.shape[0], width), jnp.float32)
    for gate_piece, up_piece, down_piece in zip(gates, ups, downs):
        gate_part = jnp.dot(flat_rows, gate_piece, preferred_element_type=jnp.float32)
        up_part = jnp.dot(flat_rows, up_piece, preferred_element_type=jnp.float32)
        hidden = (jax.nn.silu(gate_part) * up_part).astype(jnp.bfloat16)
        reduced = reduced + jnp.dot(hidden, down_piece, preferred_element_type=jnp.float32)
    results = reduced.astype(jnp.bfloat16).reshape(sources, capacity, width)
    returned = lax.all_to_all(results, "ep", split_axis=0, concat_axis=0, tiled=True)
    picked = jnp.take(returned.reshape(experts * capacity, width), target, axis=0)
    picked = picked.astype(jnp.float32).reshape(tok_count, top_count, width)
    norm_weight = route_weight / jnp.sum(route_weight, axis=1, keepdims=True)
    return jnp.sum(picked * norm_weight[:, :, None], axis=1).astype(jnp.bfloat16)


def on_device(
    mixer_input,
    mixer_gain,
    query_weight,
    key_weight,
    value_weight,
    gate_weight,
    head_gain,
    output_weight,
    log_decay,
    expert_input,
    expert_gain,
    routes,
    route_weight,
    expert_gate,
    expert_up,
    expert_down,
):
    mixer_output = mixer_half(
        mixer_input,
        mixer_gain,
        query_weight,
        key_weight,
        value_weight,
        gate_weight,
        head_gain,
        output_weight,
        log_decay,
    )
    expert_output = expert_half(
        expert_input, expert_gain, routes, route_weight, expert_gate, expert_up, expert_down
    )
    return (mixer_output, expert_output)


def solution(mesh):
    return jax.shard_map(
        on_device,
        mesh=mesh,
        in_specs=(
            P("ep", None),
            P(),
            P(None, "tp"),
            P(None, "tp"),
            P(None, "tp"),
            P(None, "tp"),
            P("tp"),
            P("tp", None),
            P("ep", "tp"),
            P(("ep", "tp"), None),
            P(),
            P(("ep", "tp"), None),
            P(("ep", "tp"), None),
            P("ep", None, "tp"),
            P("ep", None, "tp"),
            P("ep", "tp", None),
        ),
        out_specs=(P(("ep", "tp"), None), P(("ep", "tp"), None)),
        check_vma=False,
    )
```

```python
import functools

import jax
import jax.numpy as jnp
from jax import lax
from jax.experimental import pallas as pl
from jax.experimental.pallas import tpu as pltpu
from jax.sharding import PartitionSpec as P

BLOCK = 128


EPS = 1e-06
HIGH = lax.Precision.HIGHEST


def entering_kernel(n, state_ref, decay_ref, out_ref, states, decays, sent, got, sent_d, got_d):
    me = lax.axis_index("ep")
    tp = lax.axis_index("tp")
    barrier = pltpu.get_barrier_semaphore()

    def greet(offset, carry):
        pl.semaphore_signal(
            barrier,
            inc=1,
            device_id=(lax.rem(me + offset, n), tp),
            device_id_type=pl.DeviceIdType.MESH,
        )
        return carry

    lax.fori_loop(1, n, greet, 0)
    pl.semaphore_wait(barrier, n - 1)

    def copies(source, target):
        return (
            pltpu.make_async_remote_copy(
                src_ref=state_ref,
                dst_ref=states.at[source],
                send_sem=sent.at[target],
                recv_sem=got.at[source],
                device_id=(target, tp),
                device_id_type=pl.DeviceIdType.MESH,
            ),
            pltpu.make_async_remote_copy(
                src_ref=decay_ref,
                dst_ref=decays.at[source],
                send_sem=sent_d.at[target],
                recv_sem=got_d.at[source],
                device_id=(target, tp),
                device_id_type=pl.DeviceIdType.MESH,
            ),
        )

    def send(target, carry):
        for copy in copies(me, target):
            copy.start()
        return carry

    lax.fori_loop(me + 1, n, send, 0)
    out_ref[...] = jnp.zeros_like(out_ref)

    def receive(source, carry):
        for copy in copies(source, me):
            copy.wait_recv()
        for head in range(out_ref.shape[0]):
            out_ref[head] = out_ref[head] * decays[source, head, 0:1, :] + states[
                source, head
            ].astype(jnp.float32)
        return carry

    lax.fori_loop(0, me, receive, 0)

    def finish(target, carry):
        for copy in copies(me, target):
            copy.wait_send()
        return carry

    lax.fori_loop(me + 1, n, finish, 0)


def entering_state(decay, state):
    n = lax.axis_size("ep")
    heads, rows, columns = state.shape
    decay_tile = jnp.broadcast_to(decay[:, None, None], (heads, 8, columns))
    return pl.pallas_call(
        functools.partial(entering_kernel, n),
        out_shape=jax.ShapeDtypeStruct(state.shape, jnp.float32),
        in_specs=[pl.BlockSpec(memory_space=pltpu.VMEM)] * 2,
        out_specs=pl.BlockSpec(memory_space=pltpu.VMEM),
        scratch_shapes=[
            pltpu.VMEM((n, heads, rows, columns), jnp.bfloat16),
            pltpu.VMEM((n, heads, 8, columns), jnp.float32),
            pltpu.SemaphoreType.DMA((n,)),
            pltpu.SemaphoreType.DMA((n,)),
            pltpu.SemaphoreType.DMA((n,)),
            pltpu.SemaphoreType.DMA((n,)),
        ],
        compiler_params=pltpu.CompilerParams(
            collective_id=0, has_side_effects=True, vmem_limit_bytes=24 * 1024 * 1024
        ),
        cost_estimate=pl.CostEstimate(
            flops=2 * n * state.size, bytes_accessed=8 * 1024 * 1024, transcendentals=0
        ),
    )(state.astype(jnp.bfloat16), decay_tile)


def norm_rows(values, gain):
    floats = values.astype(jnp.float32)
    scale = lax.rsqrt(jnp.mean(floats * floats, axis=-1, keepdims=True) + EPS)
    return (floats * scale * gain).astype(jnp.bfloat16)


def rotate(values, position):
    half_dim = values.shape[-1] // 2
    frequency = 10000.0 ** (-jnp.arange(half_dim, dtype=jnp.float32) / half_dim)
    angles = position.astype(jnp.float32)[:, None] * frequency[None, :]
    cosine = jnp.cos(angles)[:, None, :]
    sine_part = jnp.sin(angles)[:, None, :]
    first_half = values[..., :half_dim]
    second = values[..., half_dim:]
    return jnp.concatenate(
        [first_half * cosine - second * sine_part, first_half * sine_part + second * cosine],
        axis=-1,
    )


def mixer_half(
    mixer_input,
    mixer_gain,
    query_weight,
    key_weight,
    value_weight,
    gate_weight,
    head_gain,
    output_weight,
    log_decay,
    results,
):
    row_count = mixer_input.shape[0]
    head_count = log_decay.shape[1]
    mix_width = query_weight.shape[1]
    head_dim = mix_width // head_count
    normed = norm_rows(mixer_input, mixer_gain)

    def project(weight):
        return jnp.dot(normed, weight, preferred_element_type=jnp.float32).astype(jnp.bfloat16)

    queries = project(query_weight)
    keys_raw = project(key_weight)
    values_new = project(value_weight)
    gate_raw = project(gate_weight)
    position = lax.axis_index("ep") * row_count + jnp.arange(row_count, dtype=jnp.int32)
    q_rot = rotate(
        queries.astype(jnp.float32).reshape(row_count, head_count, head_dim), position
    ).astype(jnp.bfloat16)
    k_rot = (
        rotate(keys_raw.astype(jnp.float32).reshape(row_count, head_count, head_dim), position)
        * head_dim ** (-0.5)
    ).astype(jnp.bfloat16)
    block_count = row_count // BLOCK
    q_blocks = q_rot.reshape(block_count, BLOCK, head_count, head_dim)
    k_blocks = k_rot.reshape(block_count, BLOCK, head_count, head_dim)
    v_blocks = values_new.reshape(block_count, BLOCK, head_count, head_dim)
    log_steps = log_decay.reshape(block_count, BLOCK, head_count)
    row_ids = lax.broadcasted_iota(jnp.int32, (BLOCK, BLOCK), 0)
    col_ids = lax.broadcasted_iota(jnp.int32, (BLOCK, BLOCK), 1)
    lower_mask = col_ids <= row_ids
    cumulative = jnp.einsum(
        "ij,bjh->bhi", lower_mask.astype(jnp.float32), log_steps, precision=HIGH
    )
    block_total = cumulative[:, :, -1]
    differences = cumulative[:, :, :, None] - cumulative[:, :, None, :]
    decays = jnp.where(lower_mask, jnp.exp(jnp.where(lower_mask, differences, 0.0)), 0.0)
    scores = jnp.einsum("bihd,bjhd->bhij", q_blocks, k_blocks, preferred_element_type=jnp.float32)
    weights = (scores * decays).astype(jnp.bfloat16)
    inner_term = jnp.einsum(
        "bhij,bjhe->bihe", weights, v_blocks, preferred_element_type=jnp.float32
    )
    key_scale = jnp.exp(block_total[:, :, None] - cumulative)
    updates = jnp.einsum(
        "bhj,bjhd,bjhe->bhde",
        key_scale,
        k_blocks.astype(jnp.float32),
        v_blocks.astype(jnp.float32),
        precision=HIGH,
    )
    factor = jnp.exp(block_total)
    local_state = jnp.zeros((head_count, head_dim, head_dim), jnp.float32)
    for block_index in range(block_count):
        local_state = factor[block_index][:, None, None] * local_state + updates[block_index]
    carry_state = entering_state(jnp.exp(jnp.sum(block_total, axis=0)), local_state)
    carry_state, results = lax.optimization_barrier((carry_state, results))
    starts = []
    for block_index in range(block_count):
        starts.append(carry_state)
        carry_state = factor[block_index][:, None, None] * carry_state + updates[block_index]
    carried = jnp.stack(starts)
    cross_term = jnp.einsum(
        "bhi,bihd,bhde->bihe",
        jnp.exp(cumulative),
        q_blocks.astype(jnp.float32),
        carried,
        precision=HIGH,
    )
    retained = (inner_term + cross_term).reshape(row_count, head_count, head_dim)
    centre = jnp.mean(retained, axis=-1, keepdims=True)
    spread = jnp.mean(jnp.square(retained - centre), axis=-1, keepdims=True)
    scaled = (retained - centre) * lax.rsqrt(spread + EPS) * head_gain.reshape(head_count, head_dim)
    mixer_hidden = (
        scaled.reshape(row_count, mix_width) * jax.nn.silu(gate_raw.astype(jnp.float32))
    ).astype(jnp.bfloat16)
    mixed = lax.psum_scatter(
        jnp.dot(mixer_hidden, output_weight, preferred_element_type=jnp.float32).astype(
            jnp.bfloat16
        ),
        "tp",
        scatter_dimension=0,
        tiled=True,
    )
    return mixed, results


def gathered_pieces(shard):
    peers = lax.axis_size("tp")
    pieces = [shard]
    bit = peers // 2
    while bit:
        pairs = [(i, i ^ bit) for i in range(peers)]
        pieces = pieces + [lax.ppermute(piece, "tp", pairs) for piece in pieces]
        bit //= 2
    return pieces


def expert_half(
    expert_input, expert_gain, routes, route_weight, expert_gate, expert_up, expert_down
):
    tok_count, top_count = routes.shape
    experts = lax.axis_size("ep")
    capacity = max(2, 3 * tok_count * top_count // (2 * experts))
    width = expert_input.shape[1]
    normed = norm_rows(expert_input, expert_gain)
    flat_routes = routes.reshape(-1)
    entries = flat_routes.shape[0]
    onehot = (flat_routes[:, None] == jnp.arange(experts, dtype=jnp.int32)[None, :]).astype(
        jnp.bfloat16
    )
    before = (
        lax.broadcasted_iota(jnp.int32, (entries, entries), 1)
        < lax.broadcasted_iota(jnp.int32, (entries, entries), 0)
    ).astype(jnp.bfloat16)
    prior_count = jnp.dot(before, onehot, preferred_element_type=jnp.float32)
    slot_index = jnp.sum(prior_count * onehot.astype(jnp.float32), axis=1).astype(jnp.int32)
    target = flat_routes * capacity + slot_index
    token_ids = jnp.arange(entries, dtype=jnp.int32) // top_count
    slot_table = jnp.full((experts * capacity,), tok_count, jnp.int32).at[target].set(token_ids)
    padded = jnp.concatenate([normed, jnp.zeros((1, width), jnp.bfloat16)], axis=0)
    outgoing = jnp.take(padded, slot_table, axis=0).reshape(experts, capacity, width)
    arrived = lax.all_to_all(outgoing, "ep", split_axis=0, concat_axis=0, tiled=True)
    sources = arrived.shape[0]
    flat_rows = arrived.reshape(sources * capacity, width)
    gates = gathered_pieces(expert_gate[0])
    ups = gathered_pieces(expert_up[0])
    downs = gathered_pieces(expert_down[0])
    reduced = jnp.zeros((flat_rows.shape[0], width), jnp.float32)
    for gate_piece, up_piece, down_piece in zip(gates, ups, downs):
        gate_part = jnp.dot(flat_rows, gate_piece, preferred_element_type=jnp.float32)
        up_part = jnp.dot(flat_rows, up_piece, preferred_element_type=jnp.float32)
        hidden = (jax.nn.silu(gate_part) * up_part).astype(jnp.bfloat16)
        reduced = reduced + jnp.dot(hidden, down_piece, preferred_element_type=jnp.float32)
    results = reduced.astype(jnp.bfloat16).reshape(sources, capacity, width)
    return results, target


def combine_half(results, target, route_weight):
    experts, capacity, width = results.shape
    tok_count, top_count = route_weight.shape
    returned = lax.all_to_all(results, "ep", split_axis=0, concat_axis=0, tiled=True)
    picked = jnp.take(returned.reshape(experts * capacity, width), target, axis=0)
    picked = picked.astype(jnp.float32).reshape(tok_count, top_count, width)
    norm_weight = route_weight / jnp.sum(route_weight, axis=1, keepdims=True)
    return jnp.sum(picked * norm_weight[:, :, None], axis=1).astype(jnp.bfloat16)


def on_device(
    mixer_input,
    mixer_gain,
    query_weight,
    key_weight,
    value_weight,
    gate_weight,
    head_gain,
    output_weight,
    log_decay,
    expert_input,
    expert_gain,
    routes,
    route_weight,
    expert_gate,
    expert_up,
    expert_down,
):
    results, target = expert_half(
        expert_input, expert_gain, routes, route_weight, expert_gate, expert_up, expert_down
    )
    mixer_output, results = mixer_half(
        mixer_input,
        mixer_gain,
        query_weight,
        key_weight,
        value_weight,
        gate_weight,
        head_gain,
        output_weight,
        log_decay,
        results,
    )
    expert_output = combine_half(results, target, route_weight)
    return (mixer_output, expert_output)


def solution(mesh):
    return jax.shard_map(
        on_device,
        mesh=mesh,
        in_specs=(
            P("ep", None),
            P(),
            P(None, "tp"),
            P(None, "tp"),
            P(None, "tp"),
            P(None, "tp"),
            P("tp"),
            P("tp", None),
            P("ep", "tp"),
            P(("ep", "tp"), None),
            P(),
            P(("ep", "tp"), None),
            P(("ep", "tp"), None),
            P("ep", None, "tp"),
            P("ep", None, "tp"),
            P("ep", "tp", None),
        ),
        out_specs=(P(("ep", "tp"), None), P(("ep", "tp"), None)),
        check_vma=False,
    )
```
